32 devices in a mesh: ep: 16 (over z, y, x), tp: 2 (over core).
Axes of the slice: x: 2, y: 2, z: 4, core: 2. Of those that a mesh axis runs over, the one named last changes fastest.
Arguments:
- residual_in: bfloat16 [256, 1024], P('ep'), may hold values from -6 to 6
- lengths: int32 [256], P('ep'), may hold values from 64 to 1024
- cache_keys: bfloat16 [256, 2, 1024, 128], P('ep', 'tp'), may hold values from -7 to 7
- cache_values: bfloat16 [256, 2, 1024, 128], P('ep', 'tp'), may hold values from -6 to 6
- attend_gain: bfloat16 [1024], replicated, may hold values from 0.099609375 to 1.8984375
- query_proj: bfloat16 [1024, 512], P(None, 'tp'), may hold values from -0.1875 to 0.1875
- key_proj: bfloat16 [1024, 256], P(None, 'tp'), may hold values from -0.1875 to 0.1875
- value_proj: bfloat16 [1024, 256], P(None, 'tp'), may hold values from -0.1875 to 0.1875
- lambdas: float32 [4], P('tp'), may hold values from 0.3 to 0.8
- head_gain: bfloat16 [128], replicated, may hold values from 0.099609375 to 1.8984375
- out_proj: bfloat16 [512, 1024], P('tp'), may hold values from -0.25 to 0.25
- channel_gain: bfloat16 [1024], replicated, may hold values from 0.099609375 to 1.8984375
- routes: int32 [256, 6], P('ep'), may hold values from 0 to 15, all different within a row; in each aligned block of 16 rows (0 to 15, 16 to 31, ...) at most 12 rows name the same one
- route_weight: float32 [256, 6], P('ep'), may hold values from 0.1 to 1
- expert_gate: bfloat16 [16, 1024, 512], P('ep', None, 'tp'), may hold values from -0.1875 to 0.1875
- expert_up: bfloat16 [16, 1024, 512], P('ep', None, 'tp'), may hold values from -0.1875 to 0.1875
- expert_down: bfloat16 [16, 512, 1024], P('ep', 'tp'), may hold values from -0.25 to 0.25
- dense_gate: bfloat16 [1024, 4096], P(None, ('ep', 'tp')), may hold values from -0.1875 to 0.1875
- dense_up: bfloat16 [1024, 4096], P(None, ('ep', 'tp')), may hold values from -0.1875 to 0.1875
- dense_down: bfloat16 [4096, 1024], P(('ep', 'tp')), may hold values from -0.09375 to 0.09375
- dense_mixer: bfloat16 [1024], replicated, may hold values from -0.1875 to 0.1875
Outputs:
- residual_out: bfloat16 [256, 1024], P('ep')
- new_keys: bfloat16 [256, 2, 128], P('ep', 'tp')
- new_values: bfloat16 [256, 2, 128], P('ep', 'tp')
The draws below stay inside these ranges and needn't reach their ends.
Inputs may be any that keep to these rules, and one draw needn't show every extreme that they name: `routes`: each row names 6 different experts; in each aligned block of 16 rows (the rows of one index of ep) no expert is named by more than 12 rows, and in some blocks one expert is named by exactly 12 rows.
All inputs are finite; a program needn't handle non-finite values.
Results may differ from the reference program's by a relative error of at most 0.015.
Values may be sent and summed in bfloat16 or wider, within the bound.
A program may use at most 64 MiB of HBM per device.

```python
import math
import jax
import jax.numpy as jnp
import numpy as np
from jax import lax

D = 1024
HEADS = 4
KV_HEADS = 2
HEAD = 64
VALUE = 128
EXPERT_FF = 512
DENSE_FF = 4096
TOPK = 6
SEQ_DEV = 16
LEN = 1024
TOKENS = 256
EXPERTS = 16
CAP = 12
N_EP = 16
N_TP = 2


def set_ends(values, own_key, low, high):
    index_at = [jax.random.randint(jax.random.fold_in(own_key, axis), (), 0, length) for axis, length in enumerate(values.shape)]
    longest = values.shape.index(max(values.shape))
    next_to = index_at[:longest] + [(index_at[longest] + 1) % values.shape[longest]] + index_at[longest + 1:]
    return values.at[tuple(index_at)].set(low).at[tuple(next_to)].set(high)


def block_levels(stream_key, shape, shards, smallest, largest):
    level = 1.0
    for dim, parts in shards:
        heights = jax.random.uniform(jax.random.fold_in(jax.random.fold_in(stream_key, 6), dim), (parts,), jnp.float32, smallest / len(shards), largest / len(shards))
        level = level * jnp.repeat(jnp.exp(heights), shape[dim] // parts).reshape((-1,) + (1,) * (len(shape) - 1 - dim))
    return level


def shared_out(stream_key, own, number, rows, amount, top, bound, skew):
    order = jax.random.permutation(stream_key, amount)
    heavy_load, common = load_shares(amount, rows * top, bound, skew, True), load_shares(amount, rows * top, bound, skew, False)
    places = jnp.arange(amount)

    def named(sizes, rotation):
        used = int((sizes > 0).sum())
        fixed = max(1, used // 4)
        shifted = fixed + (places - fixed + rotation * (used - fixed)) % max(1, amount - fixed)
        return jnp.zeros((amount,), jnp.int32).at[order[jnp.where(places < fixed, places, shifted)]].set(jnp.asarray(sizes, jnp.int32))

    sizes = jnp.where(number % 4 == 0, named(heavy_load, number // 4), named(common, number - number // 4 - 1))
    mixed = jax.random.permutation(jax.random.fold_in(own, 3), amount)
    donor, taker = mixed[0:amount // 2 * 2:2], mixed[1:amount // 2 * 2:2]
    room = jnp.minimum(sizes[donor] - 1, bound - sizes[taker]) // 2
    room = jnp.where((donor == order[0]) | (taker == order[0]) | (sizes[taker] == 0), 0, jnp.maximum(room, 0))
    shifted = jax.random.randint(jax.random.fold_in(own, 4), (amount // 2,), 0, 1 << 20) % (room + 1)
    sizes = sizes.at[donor].add(-shifted).at[taker].add(shifted)
    items = jnp.searchsorted(jnp.cumsum(sizes), jnp.arange(rows * top), side="right").astype(jnp.int32)
    listing = items.reshape(top, rows).T
    listing = listing[jax.random.permutation(jax.random.fold_in(own, 1), rows)]
    rotation = jax.random.randint(jax.random.fold_in(own, 2), (rows, 1), 0, top)
    return jnp.take_along_axis(listing, (jnp.arange(top)[None, :] + rotation) % top, axis=1)


def load_shares(count, total, limit, skew, full):
    loads = [(1 << 20) // math.isqrt(standing ** skew) + 1 for standing in range(1, count + 1)]
    largest = limit if full else min(limit, max(-(-total // count), total * loads[0] // sum(loads)))
    least = 1 if total - largest >= count - 1 else 0
    given, spare = [largest] + [least] * (count - 1), total - largest - least * (count - 1)
    while spare > 0:
        candidates = [i for i in range(1, count) if given[i] < largest] or [i for i in range(1, count) if given[i] < limit]
        whole, remaining = sum([loads[i] for i in candidates]), spare
        for i in candidates:
            more = min(limit - given[i], max(1, remaining * loads[i] // whole), spare)
            given[i] = given[i] + more
            spare = spare - more
    return np.array(given)


def normal_values(stream_key, shape, spread, bound, pieces=(), kind=jnp.bfloat16):
    values = spread * jax.random.normal(stream_key, shape, jnp.float32)
    if pieces:
        values = values * block_levels(stream_key, shape, pieces, -0.22, 0.18)
    return jnp.clip(values, -bound, bound).astype(kind)


def setup_inputs(seed: int = 0) -> dict:
    key_list = jax.random.split(jax.random.key(seed), 22)
    residual_in = normal_values(key_list[0], (TOKENS, D), 1.0, 6.0, ((0, 16),))
    lengths = set_ends(jax.random.randint(key_list[1], (TOKENS,), LEN // 16, LEN + 1), jax.random.fold_in(key_list[1], 1), LEN // 16, LEN).astype(jnp.int32)
    cache_keys = normal_values(key_list[2], (TOKENS, KV_HEADS, LEN, 2 * HEAD), 1.75, 7.0, ((0, 16), (1, 2)))
    cache_values = normal_values(key_list[3], (TOKENS, KV_HEADS, LEN, VALUE), 1.0, 6.0, ((0, 16), (1, 2)))
    attend_gain = jnp.clip(1.0 + 0.18 * jax.random.normal(key_list[4], (D,), jnp.float32), 0.099609375, 1.8984375).astype(jnp.bfloat16)
    query_proj = normal_values(key_list[5], (D, HEADS * 2 * HEAD), D ** -0.5, 0.1875, ((1, 2),))
    key_proj = normal_values(key_list[6], (D, KV_HEADS * 2 * HEAD), D ** -0.5, 0.1875, ((1, 2),))
    value_proj = normal_values(key_list[7], (D, KV_HEADS * VALUE), D ** -0.5, 0.1875, ((1, 2),))
    lambdas = jnp.clip(0.3 + 0.5 * jax.random.uniform(key_list[8], (HEADS,), jnp.float32) ** block_levels(key_list[8], (HEADS,), ((0, 2),), -0.2, 0.2), 0.3, 0.8)
    head_gain = jnp.clip(1.0 + 0.18 * jax.random.normal(key_list[9], (VALUE,), jnp.float32), 0.099609375, 1.8984375).astype(jnp.bfloat16)
    out_proj = normal_values(key_list[10], (HEADS * VALUE, D), (HEADS * VALUE) ** -0.5, 0.25, ((0, 2),))
    channel_gain = jnp.clip(1.0 + 0.18 * jax.random.normal(key_list[11], (D,), jnp.float32), 0.099609375, 1.8984375).astype(jnp.bfloat16)
    routes_keys = jax.random.split(jax.random.fold_in(key_list[12], 1), TOKENS // SEQ_DEV)
    routes_turns = jax.random.permutation(jax.random.fold_in(key_list[12], 3), TOKENS // SEQ_DEV)
    routes = jax.vmap(lambda own, number: shared_out(jax.random.fold_in(key_list[12], 2), own, number, SEQ_DEV, EXPERTS, TOPK, CAP, 2))(routes_keys, routes_turns).reshape((TOKENS, TOPK))
    route_weight = jnp.clip(jnp.exp(math.log(1.0) - 2.3025851 * jax.random.uniform(key_list[13], (TOKENS, TOPK), jnp.float32) ** block_levels(key_list[13], (TOKENS, TOPK), ((0, 16),), -0.2, 0.2)), 0.1, 1.0)
    expert_gate = normal_values(key_list[14], (EXPERTS, D, EXPERT_FF), D ** -0.5, 0.1875, ((0, 16), (2, 2)))
    expert_up = normal_values(key_list[15], (EXPERTS, D, EXPERT_FF), D ** -0.5, 0.1875, ((0, 16), (2, 2)))
    expert_down = normal_values(key_list[16], (EXPERTS, EXPERT_FF, D), EXPERT_FF ** -0.5, 0.25, ((0, 16), (1, 2)))
    dense_gate = normal_values(key_list[17], (D, DENSE_FF), D ** -0.5, 0.1875, ((1, 32),))
    dense_up = normal_values(key_list[18], (D, DENSE_FF), D ** -0.5, 0.1875, ((1, 32),))
    dense_down = normal_values(key_list[19], (DENSE_FF, D), DENSE_FF ** -0.5, 0.09375, ((0, 32),))
    dense_mixer = normal_values(key_list[20], (D,), D ** -0.5, 0.1875)
    return {"residual_in": residual_in, "lengths": lengths, "cache_keys": cache_keys, "cache_values": cache_values, "attend_gain": attend_gain, "query_proj": query_proj, "key_proj": key_proj, "value_proj": value_proj, "lambdas": lambdas, "head_gain": head_gain, "out_proj": out_proj, "channel_gain": channel_gain, "routes": routes, "route_weight": route_weight, "expert_gate": expert_gate, "expert_up": expert_up, "expert_down": expert_down, "dense_gate": dense_gate, "dense_up": dense_up, "dense_down": dense_down, "dense_mixer": dense_mixer}


NORM_EPSILON = 1e-06
ROTARY_BASE = 10000.0
HEAD_SCALE = 0.8

def norm_scale(vectors, gain_vector):
    mean_square = lax.optimization_barrier(jnp.mean(vectors * vectors, axis=-1, keepdims=True))
    return vectors * lax.rsqrt(mean_square + NORM_EPSILON) * gain_vector

def rotate(vectors, position):
    half_width = vectors.shape[-1] // 2
    inverse = ROTARY_BASE ** (-jnp.arange(half_width, dtype=jnp.float32) / half_width)
    angles = position[..., None] * inverse
    cosine = jnp.cos(angles)
    sine_part = jnp.sin(angles)
    front_half = vectors[..., :half_width]
    back_half = vectors[..., half_width:]
    return jnp.concatenate([front_half * cosine - back_half * sine_part, back_half * cosine + front_half * sine_part], axis=-1)

def rounded(values):
    return lax.optimization_barrier(values.astype(jnp.bfloat16)).astype(jnp.float32)

def reference(residual_in, lengths, cache_keys, cache_values, attend_gain, query_proj, key_proj, value_proj, lambdas, head_gain, out_proj, channel_gain, routes, route_weight, expert_gate, expert_up, expert_down, dense_gate, dense_up, dense_down, dense_mixer):
    residual = residual_in.astype(jnp.float32)
    normed = norm_scale(residual, attend_gain.astype(jnp.float32)).astype(jnp.bfloat16)
    queries = jnp.dot(normed, query_proj, preferred_element_type=jnp.float32).reshape(TOKENS, HEADS, 2, HEAD)
    key_rows = jnp.dot(normed, key_proj, preferred_element_type=jnp.float32).reshape(TOKENS, KV_HEADS, 2, HEAD)
    new_values = jnp.dot(normed, value_proj, preferred_element_type=jnp.float32).astype(jnp.bfloat16).reshape(TOKENS, KV_HEADS, VALUE)
    position = lengths.astype(jnp.float32)[:, None, None]
    queries = rotate(queries, position).astype(jnp.bfloat16)
    new_keys = rotate(key_rows, position).astype(jnp.bfloat16)
    group_size = HEADS // KV_HEADS
    mixing = lambdas.astype(jnp.float32).reshape(KV_HEADS, group_size)[None, :, :, None]
    score_scale = HEAD ** (-0.5)

    def attend(block):
        block_queries, block_keys, block_values, cached_keys, cached_values, block_lengths = block
        grouped = block_queries.astype(jnp.float32).reshape(SEQ_DEV, KV_HEADS, group_size, 2, HEAD)
        cached = cached_keys.astype(jnp.float32).reshape(SEQ_DEV, KV_HEADS, LEN, 2, HEAD)
        scores = jnp.einsum('sagmd,salmd->sagml', grouped, cached) * score_scale
        own_score = jnp.einsum('sagmd,samd->sagm', grouped, block_keys.astype(jnp.float32)) * score_scale
        visible = (jnp.arange(LEN).astype(jnp.int32)[None, :] < block_lengths.astype(jnp.int32)[:, None])[:, None, None, None, :]
        exponent = jnp.where(visible, jnp.exp(scores), 0.0)
        own_exponent = jnp.exp(own_score)
        denominator = lax.optimization_barrier(jnp.sum(exponent, axis=-1)) + own_exponent
        probability = exponent / denominator[..., None]
        own_probability = own_exponent / denominator
        weight = (probability[..., 0, :] - mixing * probability[..., 1, :]).astype(jnp.bfloat16)
        own_weight = (own_probability[..., 0] - mixing[..., 0] * own_probability[..., 1]).astype(jnp.bfloat16)
        attended = jnp.einsum('sagl,sale->sage', weight.astype(jnp.float32), cached_values.astype(jnp.float32))
        return attended + own_weight.astype(jnp.float32)[..., None] * block_values.astype(jnp.float32)[:, :, None, :]
    blocks = (queries.reshape(N_EP, SEQ_DEV, HEADS, 2, HEAD), new_keys.reshape(N_EP, SEQ_DEV, KV_HEADS, 2, HEAD), new_values.reshape(N_EP, SEQ_DEV, KV_HEADS, VALUE), cache_keys.reshape(N_EP, SEQ_DEV, KV_HEADS, LEN, 2 * HEAD), cache_values.reshape(N_EP, SEQ_DEV, KV_HEADS, LEN, VALUE), lengths.reshape(N_EP, SEQ_DEV))
    attended = lax.map(attend, blocks).reshape(TOKENS, KV_HEADS, group_size, VALUE)
    head_rows = (norm_scale(attended, head_gain.astype(jnp.float32)) * HEAD_SCALE).astype(jnp.bfloat16).reshape(TOKENS, HEADS * VALUE)
    part_width = HEADS * VALUE // N_TP
    attend_out = jnp.zeros((TOKENS, D), jnp.float32)
    for core in range(N_TP):
        head_part = head_rows[:, core * part_width:(core + 1) * part_width]
        attend_out = attend_out + rounded(jnp.dot(head_part, out_proj[core * part_width:(core + 1) * part_width], preferred_element_type=jnp.float32))
    middle = (residual + attend_out).astype(jnp.bfloat16)
    normed_second = norm_scale(middle.astype(jnp.float32), channel_gain.astype(jnp.float32)).astype(jnp.bfloat16)
    dense_gated = jnp.dot(normed_second, dense_gate, preferred_element_type=jnp.float32)
    dense_upper = jnp.dot(normed_second, dense_up, preferred_element_type=jnp.float32)
    dense_hidden = (jax.nn.silu(dense_gated) * dense_upper).astype(jnp.bfloat16)
    dense_out = jnp.dot(dense_hidden, dense_down, preferred_element_type=jnp.float32)
    switch = jax.nn.sigmoid(jnp.dot(normed_second, dense_mixer, preferred_element_type=jnp.float32))
    pair_routes = routes.astype(jnp.int32).reshape(N_EP, SEQ_DEV * TOPK)
    onehot = (pair_routes[..., None] == jnp.arange(EXPERTS).astype(jnp.int32)[None, None, :]).astype(jnp.int32)
    slot_index = lax.optimization_barrier(jnp.sum((jnp.cumsum(onehot, axis=1) - onehot) * onehot, axis=-1)).astype(jnp.int32)
    source_ids = jnp.arange(N_EP).astype(jnp.int32)[:, None]
    placement = (pair_routes * (N_EP * CAP) + source_ids * CAP + slot_index).reshape(TOKENS * TOPK).astype(jnp.int32)
    token_ids = (jnp.arange(TOKENS * TOPK) // TOPK).astype(jnp.int32)
    slot_table = jnp.zeros((EXPERTS * N_EP * CAP,), jnp.int32).at[placement].set(token_ids).reshape(EXPERTS, N_EP * CAP)
    half_units = EXPERT_FF // N_TP

    def run_expert(expert_item):
        row_index, gate_weight, up_weight, down_weight = expert_item
        routed_rows = normed_second[row_index]
        gated = jnp.dot(routed_rows, gate_weight, preferred_element_type=jnp.float32)
        upper = jnp.dot(routed_rows, up_weight, preferred_element_type=jnp.float32)
        hidden = (jax.nn.silu(gated) * upper).astype(jnp.bfloat16)
        output = jnp.zeros((N_EP * CAP, D), jnp.float32)
        for core in range(N_TP):
            output = output + rounded(jnp.dot(hidden[:, core * half_units:(core + 1) * half_units], down_weight[core * half_units:(core + 1) * half_units], preferred_element_type=jnp.float32))
        return output.astype(jnp.bfloat16)
    expert_rows = lax.map(run_expert, (slot_table, expert_gate, expert_up, expert_down))
    picked = expert_rows.reshape(EXPERTS * N_EP * CAP, D)[placement].astype(jnp.float32).reshape(TOKENS, TOPK, D)
    routed = lax.optimization_barrier(jnp.sum(picked * route_weight.astype(jnp.float32)[..., None], axis=1))
    residual_out = (middle.astype(jnp.float32) + routed + switch[:, None] * dense_out).astype(jnp.bfloat16)
    return (residual_out, new_keys.reshape(TOKENS, KV_HEADS, 2 * HEAD), new_values)
```

```python
import functools

import jax
import jax.numpy as jnp
import numpy as np
from jax import lax
from jax.experimental import pallas as pl
from jax.experimental.pallas import tpu as pltpu
from jax.sharding import PartitionSpec as P

HEAD = 64
NORM_EPSILON = 1e-06
ROTARY_BASE = 10000.0
HEAD_SCALE = 0.8
KEY_CHUNKS = 4
MESH = pl.DeviceIdType.MESH
F32 = jnp.float32
BF16 = jnp.bfloat16


def norm_scale(vectors, gain_vector):
    mean_square = jnp.mean(vectors * vectors, axis=-1, keepdims=True)
    return vectors * lax.rsqrt(mean_square + NORM_EPSILON) * gain_vector


def mm(a, b):
    return jnp.dot(a, b, preferred_element_type=F32)


def row_of(ref):
    return ref[...].astype(F32).reshape(1, ref.shape[0])


def silu(v):
    return v / (1.0 + jnp.exp(-v))


def kernel(
    n,
    len_hbm,
    lam_hbm,
    inv_hbm,
    res_hbm,
    again_hbm,
    hgain_hbm,
    cgain_hbm,
    mixer_hbm,
    routes_hbm,
    rw_hbm,
    ck_hbm,
    cv_hbm,
    wq_hbm,
    wk_hbm,
    wv_hbm,
    wo_hbm,
    eg_hbm,
    eu_hbm,
    ed_hbm,
    dg_hbm,
    du_hbm,
    dd_hbm,
    out_ref,
    nk_ref,
    nv_ref,
    lens,
    lam,
    inv,
    res,
    again,
    hgain,
    cgain,
    mixer,
    routes_v,
    rw_v,
    ck,
    cv,
    wq,
    wk,
    wv,
    wo,
    eg,
    eu,
    ed,
    dg,
    du,
    dd,
    pos,
    qs,
    es,
    den,
    att,
    part,
    part_in,
    mid,
    tabf,
    tab,
    xs,
    ys,
    rs,
    ob,
    small_sem,
    proj_sem,
    key_sem,
    val_sem,
    own_sem,
    wsend,
    wrecv,
    link,
):
    seqs, width = res.shape
    half = xs.shape[1]
    me = lax.axis_index("ep")
    tp = lax.axis_index("tp")
    other = 1 - tp
    chunk = seqs // KEY_CHUNKS

    small = [
        pltpu.make_async_copy(a, b, small_sem.at[i])
        for i, (a, b) in enumerate(
            (
                (len_hbm, lens),
                (inv_hbm, inv),
                (res_hbm, res),
                (again_hbm, again),
                (routes_hbm, routes_v),
                (rw_hbm, rw_v),
                (lam_hbm, lam),
                (hgain_hbm, hgain),
                (cgain_hbm, cgain),
                (mixer_hbm, mixer),
            )
        )
    ]
    proj = [
        pltpu.make_async_copy(a, b, proj_sem.at[i])
        for i, (a, b) in enumerate(((wq_hbm, wq), (wk_hbm, wk), (wv_hbm, wv), (wo_hbm, wo)))
    ]
    keys = [
        pltpu.make_async_copy(
            ck_hbm.at[pl.ds(i * chunk, chunk)], ck.at[pl.ds(i * chunk, chunk)], key_sem.at[i]
        )
        for i in range(KEY_CHUNKS)
    ]
    vals = [
        pltpu.make_async_copy(
            cv_hbm.at[pl.ds(i * chunk, chunk)], cv.at[pl.ds(i * chunk, chunk)], val_sem.at[i]
        )
        for i in range(KEY_CHUNKS)
    ]
    weight_pairs = (
        (eg_hbm, eg),
        (eu_hbm, eu),
        (ed_hbm, ed),
        (dg_hbm, dg),
        (du_hbm, du),
        (dd_hbm, dd),
    )
    own = [
        pltpu.make_async_copy(a, b.at[0], own_sem.at[i]) for i, (a, b) in enumerate(weight_pairs)
    ]
    for c in small[:4] + proj[:3] + keys[:1] + small[4:] + keys[1:2]:
        c.start()

    bar = pltpu.get_barrier_semaphore()
    pl.semaphore_signal(bar, inc=1, device_id=(me, other), device_id_type=MESH)

    def greet(k, c):
        pl.semaphore_signal(
            bar, inc=1, device_id=(lax.rem(me + k, n), tp), device_id_type=MESH
        )
        return c

    lax.fori_loop(1, n, greet, 0)

    small[0].wait()
    for s in range(seqs):
        pos[s : s + 1, :] = jnp.full((1, 2 * HEAD), lens[s].astype(F32), F32)
    small[1].wait()
    angles = pos[...] * inv[...]
    cosine = jnp.cos(angles)
    lane = lax.broadcasted_iota(jnp.int32, (seqs, 2 * HEAD), 1)
    front = (lane % HEAD) < HEAD // 2
    sine = jnp.where(front, -1.0, 1.0) * jnp.sin(angles)

    def rotate(u):
        swapped = jnp.where(
            front,
            pltpu.roll(u, 2 * HEAD - HEAD // 2, 1),
            pltpu.roll(u, HEAD // 2, 1),
        )
        return (u * cosine + swapped * sine).astype(BF16)

    small[2].wait()
    small[3].wait()
    residual = res[...].astype(F32)
    normed = norm_scale(residual, row_of(again)).astype(BF16)
    for c in proj[:3]:
        c.wait()
    for c in vals[:2] + proj[3:]:
        c.start()
    queries = mm(normed, wq[...])
    new_keys = rotate(mm(normed, wk[...]))
    new_values = mm(normed, wv[...]).astype(BF16)
    nk_ref[...] = new_keys
    nv_ref[...] = new_values
    groups = queries.shape[1] // (2 * HEAD)
    rows = qs.shape[1]
    qs[...] = jnp.zeros_like(qs)
    for g in range(groups):
        turned = rotate(queries[:, g * 2 * HEAD : (g + 1) * 2 * HEAD]).astype(F32) * (
            HEAD**-0.5
        )
        for m in range(2):
            qs[:, 2 * g + m, :] = jnp.where(lane // HEAD == m, turned, 0.0)

    for c in small[4:]:
        c.wait()
    lanes = tabf.shape[1]
    expert_row = lax.broadcasted_iota(jnp.int32, (lanes, seqs), 0)
    routes = routes_v[...]
    rweights = rw_v[...]
    table = jnp.zeros((lanes, seqs), F32)
    for k in range(routes.shape[0]):
        table = table + jnp.where(expert_row == routes[k : k + 1], rweights[k : k + 1], 0.0)
    tabf[...] = table.T
    mine = pl.ds(pl.multiple_of(tp * half, half), half)
    tab[me] = tabf[mine, :]

    def to_peer(src, dst, k, peer):
        return pltpu.make_async_remote_copy(
            src_ref=src,
            dst_ref=dst,
            send_sem=link.at[2 * k],
            recv_sem=link.at[2 * k + 1],
            device_id=peer,
            device_id_type=MESH,
        )

    def each_peer(send):
        if n & (n - 1) == 0 and n <= 16:
            bits = [lax.rem(lax.div(me, 1 << b), 2) for b in range(n.bit_length() - 1)]
            for k in range(n - 1, 0, -1):
                send(
                    sum(
                        (1 << b) * (1 - bit if k >> b & 1 else bit)
                        for b, bit in enumerate(bits)
                    )
                )
        else:

            def step(k, c):
                send(lax.rem(me + k, n))
                return c

            lax.fori_loop(1, n, step, 0)

    def all_but_one(buffer, k):
        block = buffer.at[pl.ds(0, n - 1)]
        return to_peer(block, block, k, (me, other))

    pl.semaphore_wait(bar, n)
    swaps = [
        pltpu.make_async_remote_copy(
            src_ref=a,
            dst_ref=b.at[1],
            send_sem=wsend.at[i],
            recv_sem=wrecv.at[i],
            device_id=(me, other),
            device_id_type=MESH,
        )
        for i, (a, b) in enumerate(weight_pairs)
    ]
    for i in (0, 1):
        own[i].start()
        swaps[i].start()
    each_peer(lambda peer: to_peer(tab.at[me], tab.at[me], 0, (peer, tp)).start())

    position = lax.broadcasted_iota(jnp.int32, (rows, ck.shape[1]), 1)
    kf = new_keys.astype(F32).reshape(seqs, 1, 2 * HEAD)
    vf = new_values.astype(F32).reshape(seqs, 1, new_values.shape[1])
    own_exp = jnp.exp(jnp.sum(qs[...] * kf, axis=-1, keepdims=True))
    head_gain = row_of(hgain)

    def score(g):
        for s in range(g * half, (g + 1) * half):
            if s % chunk == 0:
                keys[s // chunk].wait()
                if s // chunk + 2 < KEY_CHUNKS:
                    keys[s // chunk + 2].start()
            scores = lax.dot_general(
                qs[s].astype(BF16), ck[s], (((1,), (1,)), ((), ())), preferred_element_type=F32
            )
            exponent = jnp.where(position < lens[s], jnp.exp(scores), 0.0)
            den[s] = jnp.broadcast_to(
                jnp.sum(exponent, axis=-1, keepdims=True), den.shape[1:]
            )
            es[s] = exponent.astype(BF16)

    def attend(g):
        mine = slice(g * half, (g + 1) * half)
        for s in range(g * half, (g + 1) * half):
            if s % chunk == 0:
                vals[s // chunk].wait()
                if s // chunk + 2 < KEY_CHUNKS:
                    vals[s // chunk + 2].start()
            att[s] = mm(es[s], cv[s])
        here = own_exp[mine]
        att[mine] = (att[mine] + here * vf[mine]) / (den[mine] + here)
        if g == 0:
            proj[3].wait()
        heads = [
            (
                norm_scale(
                    att[mine, 2 * h, :] - lam[h] * att[mine, 2 * h + 1, :], head_gain
                )
                * HEAD_SCALE
            ).astype(BF16)
            for h in range(groups)
        ]
        part[g] = mm(jnp.concatenate(heads, axis=1), wo[...]).astype(BF16)

    swap = to_peer(part.at[other], part_in, 1, (me, other))

    def finish(g):
        swap.wait_recv()
        middle = residual[g * half : (g + 1) * half] + (
            part[g].astype(F32) + part_in[...].astype(F32)
        )
        middle = middle.astype(BF16).astype(F32)
        mid[...] = middle
        xs[me] = norm_scale(middle, row_of(cgain)).astype(BF16)
        each_peer(lambda peer: to_peer(xs.at[me], xs.at[me], 2, (peer, tp)).start())

    score(0)
    attend(0)

    @pl.when(tp == 1)
    def _():
        swap.start()

    score(1)

    @pl.when(tp == 0)
    def _():
        finish(0)

    attend(1)

    @pl.when(tp == 0)
    def _():
        swap.start()

    for i in (2, 3, 4, 5):
        own[i].start()
        swaps[i].start()

    @pl.when(tp == 1)
    def _():
        finish(1)

    swap.wait_send()
    for c in own:
        c.wait()
    for c in swaps:
        c.wait()
    all_but_one(tab, 0).wait()
    all_but_one(xs, 2).wait()

    count = n * half
    xf = xs[...].astype(F32).reshape(count, width)
    x = xf.astype(BF16)
    switch = 1.0 / (
        1.0 + jnp.exp(-jnp.sum(xf * row_of(mixer), axis=-1, keepdims=True))
    )
    table_all = tab[...].reshape(count, lanes)
    weight = jnp.sum(
        jnp.where(lax.broadcasted_iota(jnp.int32, (count, lanes), 1) == me, table_all, 0.0),
        axis=-1,
        keepdims=True,
    )
    total = None
    for gate, up, down, scale in ((eg, eu, ed, weight), (dg, du, dd, switch)):
        units = gate.shape[2]
        merge = units % 128 == 0
        for slots in ((0, 1),) if merge else ((0,), (1,)):
            gw = jnp.concatenate([gate[i] for i in slots], axis=1) if merge else gate[slots[0]]
            uw = jnp.concatenate([up[i] for i in slots], axis=1) if merge else up[slots[0]]
            dw = jnp.concatenate([down[i] for i in slots], axis=0) if merge else down[slots[0]]
            hidden = (silu(mm(x, gw)) * mm(x, uw) * scale).astype(BF16)
            term = mm(hidden, dw)
            total = term if total is None else total + term
    ys[...] = total.reshape(n, half, width).astype(BF16)
    rs[me] = ys[me]
    each_peer(lambda peer: to_peer(ys.at[peer], rs.at[me], 3, (peer, tp)).start())
    all_but_one(ys, 3).wait()
    ob[tp] = (mid[...] + jnp.sum(rs[...].astype(F32), axis=0)).astype(BF16)
    last = to_peer(ob.at[tp], ob.at[tp], 4, (me, other))
    last.start()
    last.wait()
    out_ref[...] = ob[...].astype(F32).reshape(seqs, width).astype(BF16)


def hand_over(*refs):
    count = (len(refs) - 1) // 2
    sem = refs[-1]
    copies = [
        pltpu.make_async_copy(source, target, sem.at[i])
        for i, (source, target) in enumerate(zip(refs[:count], refs[count : 2 * count]))
    ]
    for c in copies:
        c.start()
    for c in copies:
        c.wait()


def per_device(
    n,
    residual_in,
    lengths,
    cache_keys,
    cache_values,
    attend_gain,
    query_proj,
    key_proj,
    value_proj,
    lambdas,
    head_gain,
    out_proj,
    channel_gain,
    routes,
    route_weight,
    expert_gate,
    expert_up,
    expert_down,
    dense_gate,
    dense_up,
    dense_down,
    dense_mixer,
):
    seqs, width = residual_in.shape
    _, kv_local, length, key_width = cache_keys.shape
    value_width = cache_values.shape[3]
    half = seqs // 2
    lanes = -(-n // 128) * 128
    rows = 8
    inverse = ROTARY_BASE ** (-np.arange(HEAD // 2, dtype=np.float32) / (HEAD // 2))
    inverse = jnp.asarray(np.tile(inverse.astype(np.float32), 4)[None, :])
    vmem = pl.BlockSpec(memory_space=pltpu.VMEM)
    hbm = pl.BlockSpec(memory_space=pltpu.HBM)

    def two(w):
        return pltpu.VMEM((2,) + w.shape, BF16)

    eg, eu, ed = expert_gate[0], expert_up[0], expert_down[0]
    small = (
        lengths,
        lambdas,
        inverse,
        residual_in,
        attend_gain,
        head_gain,
        channel_gain,
        dense_mixer,
        routes.T,
        route_weight.T,
    )
    big = (
        cache_keys.reshape(seqs, length, key_width),
        cache_values.reshape(seqs, length, value_width),
        query_proj,
        key_proj,
        value_proj,
        out_proj,
        eg,
        eu,
        ed,
        dense_gate,
        dense_up,
        dense_down,
    )
    dma = pltpu.SemaphoreType.DMA
    results = ((seqs, width), (seqs, key_width), (seqs, value_width))
    out, nk, nv = pl.pallas_call(
        functools.partial(kernel, n),
        out_shape=tuple(pltpu.VMEM(shape, BF16) for shape in results),
        in_specs=[hbm] * (len(small) + len(big)),
        out_specs=(vmem, vmem, vmem),
        scratch_shapes=[pltpu.SMEM(a.shape, a.dtype) for a in small[:2]]
        + [pltpu.VMEM(a.shape, a.dtype) for a in small[2:]]
        + [pltpu.VMEM(w.shape, BF16) for w in big[:6]]
        + [two(w) for w in big[6:]]
        + [
            pltpu.VMEM((seqs, 2 * HEAD), F32),
            pltpu.VMEM((seqs, rows, key_width), F32),
            pltpu.VMEM((seqs, rows, length), BF16),
            pltpu.VMEM((seqs, rows, value_width), F32),
            pltpu.VMEM((seqs, rows, value_width), F32),
            pltpu.VMEM((2, half, width), BF16),
            pltpu.VMEM((half, width), BF16),
            pltpu.VMEM((half, width), F32),
            pltpu.VMEM((seqs, lanes), F32),
            pltpu.VMEM((n, half, lanes), F32),
            pltpu.VMEM((n, half, width), BF16),
            pltpu.VMEM((n, half, width), BF16),
            pltpu.VMEM((n, half, width), BF16),
            pltpu.VMEM((2, half, width), BF16),
            dma((len(small),)),
            dma((4,)),
            dma((KEY_CHUNKS,)),
            dma((KEY_CHUNKS,)),
            dma((6,)),
            dma((6,)),
            dma((6,)),
            dma((10,)),
        ],
        compiler_params=pltpu.CompilerParams(
            collective_id=0, has_side_effects=True, vmem_limit_bytes=56 * 1024 * 1024
        ),
    )(*(pltpu.with_memory_space_constraint(a, pltpu.HBM) for a in small + big))
    out, nk, nv = pl.pallas_call(
        hand_over,
        out_shape=tuple(jax.ShapeDtypeStruct(shape, BF16) for shape in results),
        in_specs=[vmem] * 3,
        out_specs=(hbm, hbm, hbm),
        scratch_shapes=[dma((3,))],
        compiler_params=pltpu.CompilerParams(vmem_limit_bytes=1024 * 1024),
    )(out, nk, nv)
    return (
        out,
        nk.reshape(seqs, kv_local, key_width),
        nv.reshape(seqs, kv_local, value_width),
    )


def solution(mesh):
    return jax.shard_map(
        functools.partial(per_device, mesh.shape["ep"]),
        mesh=mesh,
        in_specs=(
            P("ep", None),
            P("ep"),
            P("ep", "tp", None, None),
            P("ep", "tp", None, None),
            P(),
            P(None, "tp"),
            P(None, "tp"),
            P(None, "tp"),
            P("tp"),
            P(),
            P("tp", None),
            P(),
            P("ep", None),
            P("ep", None),
            P("ep", None, "tp"),
            P("ep", None, "tp"),
            P("ep", "tp", None),
            P(None, ("ep", "tp")),
            P(None, ("ep", "tp")),
            P(("ep", "tp"), None),
            P(),
        ),
        out_specs=(P("ep", None), P("ep", "tp", None), P("ep", "tp", None)),
        check_vma=False,
    )
```

```python
import functools

import jax
import jax.numpy as jnp
import numpy as np
from jax import lax
from jax.experimental import pallas as pl
from jax.experimental.pallas import tpu as pltpu
from jax.sharding import PartitionSpec as P

HEAD = 64
NORM_EPSILON = 1e-06
ROTARY_BASE = 10000.0
HEAD_SCALE = 0.8
KEY_CHUNKS = 4
PASSES = 4
MESH = pl.DeviceIdType.MESH
F32 = jnp.float32
BF16 = jnp.bfloat16


def norm_scale(vectors, gain_vector):
    mean_square = jnp.mean(vectors * vectors, axis=-1, keepdims=True)
    return vectors * lax.rsqrt(mean_square + NORM_EPSILON) * gain_vector


def mm(a, b):
    return jnp.dot(a, b, preferred_element_type=F32)


def row_of(ref):
    return ref[...].astype(F32).reshape(1, ref.shape[0])


def silu(v):
    return v / (1.0 + jnp.exp(-v))


def kernel(
    n,
    len_hbm,
    lam_hbm,
    inv_hbm,
    res_hbm,
    again_hbm,
    hgain_hbm,
    cgain_hbm,
    mixer_hbm,
    routes_hbm,
    rw_hbm,
    ck_hbm,
    cv_hbm,
    wq_hbm,
    wk_hbm,
    wv_hbm,
    wo_hbm,
    eg_hbm,
    eu_hbm,
    ed_hbm,
    dg_hbm,
    du_hbm,
    dd_hbm,
    out_ref,
    nk_ref,
    nv_ref,
    lens,
    lam,
    inv,
    res,
    again,
    hgain,
    cgain,
    mixer,
    routes_v,
    rw_v,
    ck,
    cv,
    wq,
    wk,
    wv,
    wo,
    eg,
    eu,
    ed,
    dg,
    du,
    dd,
    pos,
    resf,
    knew,
    vnew,
    qs,
    es,
    den,
    att,
    part,
    part_in,
    mid,
    tabf,
    tab,
    xs,
    ys,
    rs,
    ob,
    small_sem,
    proj_sem,
    key_sem,
    val_sem,
    own_sem,
    wsend,
    wrecv,
    sent,
    got,
):
    seqs, width = res.shape
    half = xs.shape[1]
    me = lax.axis_index("ep")
    tp = lax.axis_index("tp")
    other = 1 - tp
    chunk = seqs // KEY_CHUNKS
    reach = n // PASSES
    my_part = lax.div(me, reach)

    def part_of(i):
        group = other if i < KEY_CHUNKS // 2 else tp
        return pl.ds(group * half + i % (KEY_CHUNKS // 2) * chunk, chunk)

    def rows_of(group):
        return pl.ds(pl.multiple_of(group * half, half), half)

    small = [
        pltpu.make_async_copy(a, b, small_sem.at[i])
        for i, (a, b) in enumerate(
            (
                (len_hbm, lens),
                (inv_hbm, inv),
                (res_hbm, res),
                (again_hbm, again),
                (routes_hbm, routes_v),
                (rw_hbm, rw_v),
                (lam_hbm, lam),
                (hgain_hbm, hgain),
                (cgain_hbm, cgain),
                (mixer_hbm, mixer),
            )
        )
    ]
    proj = [
        pltpu.make_async_copy(a, b, proj_sem.at[i])
        for i, (a, b) in enumerate(((wq_hbm, wq), (wk_hbm, wk), (wv_hbm, wv), (wo_hbm, wo)))
    ]
    keys = [
        pltpu.make_async_copy(ck_hbm.at[part_of(i)], ck.at[part_of(i)], key_sem.at[i])
        for i in range(KEY_CHUNKS)
    ]
    vals = [
        pltpu.make_async_copy(cv_hbm.at[part_of(i)], cv.at[part_of(i)], val_sem.at[i])
        for i in range(KEY_CHUNKS)
    ]
    weight_pairs = (
        (eg_hbm, eg),
        (eu_hbm, eu),
        (ed_hbm, ed),
        (dg_hbm, dg),
        (du_hbm, du),
        (dd_hbm, dd),
    )
    own = [
        pltpu.make_async_copy(a, b.at[0], own_sem.at[i]) for i, (a, b) in enumerate(weight_pairs)
    ]
    for c in small[:4] + proj[:3] + small[4:]:
        c.start()

    bar = pltpu.get_barrier_semaphore()
    pl.semaphore_signal(bar, inc=1, device_id=(me, other), device_id_type=MESH)

    def greet(k, c):
        pl.semaphore_signal(
            bar, inc=1, device_id=(lax.rem(me + k, n), tp), device_id_type=MESH
        )
        return c

    lax.fori_loop(1, n, greet, 0)
    keys[0].start()

    small[0].wait()
    for s in range(seqs):
        pos[s : s + 1, :] = jnp.full((1, 2 * HEAD), lens[s].astype(F32), F32)
    small[1].wait()
    angles = pos[...] * inv[...]
    cosine = jnp.cos(angles)
    lane = lax.broadcasted_iota(jnp.int32, (seqs, 2 * HEAD), 1)
    front = (lane % HEAD) < HEAD // 2
    sine = jnp.where(front, -1.0, 1.0) * jnp.sin(angles)

    def rotate(u):
        swapped = jnp.where(
            front,
            pltpu.roll(u, 2 * HEAD - HEAD // 2, 1),
            pltpu.roll(u, HEAD // 2, 1),
        )
        return (u * cosine + swapped * sine).astype(BF16)

    small[2].wait()
    small[3].wait()
    for c in keys[1:2] + vals[:2]:
        c.start()
    resf[...] = res[...].astype(F32)
    normed = norm_scale(resf[...], row_of(again)).astype(BF16)
    for c in small[4:]:
        c.wait()
    expert_row = lax.broadcasted_iota(jnp.int32, (n, 1, seqs), 0)
    routes = routes_v[...].reshape(-1, 1, 1, seqs)
    rweights = rw_v[...].reshape(-1, 1, 1, seqs)
    table = jnp.zeros((n, 1, seqs), F32)
    for k in range(routes.shape[0]):
        table = table + jnp.where(expert_row == routes[k], rweights[k], 0.0)
    tabf[...] = jnp.zeros_like(tabf)
    tabf[:, :, 0:seqs] = table
    tab[me] = tabf[me]
    for c in proj[:3]:
        c.wait()
    for c in keys[2:] + proj[3:]:
        c.start()
    queries = mm(normed, wq[...])
    new_keys = rotate(mm(normed, wk[...]))
    new_values = mm(normed, wv[...]).astype(BF16)
    nk_ref[...] = new_keys
    nv_ref[...] = new_values
    knew[...] = new_keys.astype(F32)
    vnew[...] = new_values.astype(F32)
    groups = queries.shape[1] // (2 * HEAD)
    rows = qs.shape[1]
    qs[...] = jnp.zeros_like(qs)
    for g in range(groups):
        turned = rotate(queries[:, g * 2 * HEAD : (g + 1) * 2 * HEAD]).astype(F32) * (
            HEAD**-0.5
        )
        for m in range(2):
            qs[:, 2 * g + m, :] = jnp.where(lane // HEAD == m, turned, 0.0)

    def to_peer(src, dst, k, peer, r=None):
        return pltpu.make_async_remote_copy(
            src_ref=src,
            dst_ref=dst,
            send_sem=sent.at[k],
            recv_sem=got.at[k if r is None else r],
            device_id=peer,
            device_id_type=MESH,
        )

    low = lax.rem(me, reach)

    def each_peer(send, h):
        if reach & (reach - 1) == 0 and reach <= 8:
            bits = [lax.rem(lax.div(low, 1 << b), 2) for b in range(reach.bit_length() - 1)]
            for k in range(reach - 1, 0, -1):
                send(
                    h * reach
                    + sum(
                        (1 << b) * (1 - bit if k >> b & 1 else bit)
                        for b, bit in enumerate(bits)
                    )
                )
        else:

            def step(k, c):
                send(h * reach + lax.rem(low + k, reach))
                return c

            lax.fori_loop(1, reach, step, 0)

        @pl.when(my_part != h)
        def _():
            send(h * reach + low)

    def blocks(buffer, count, k, r=None):
        block = buffer.at[pl.ds(0, count)]
        return to_peer(block, block, k, (me, other), r)

    swaps = [
        pltpu.make_async_remote_copy(
            src_ref=a,
            dst_ref=b.at[1],
            send_sem=wsend.at[i],
            recv_sem=wrecv.at[i],
            device_id=(me, other),
            device_id_type=MESH,
        )
        for i, (a, b) in enumerate(weight_pairs)
    ]
    position = lax.broadcasted_iota(jnp.int32, (rows, ck.shape[1]), 1)
    head_gain = row_of(hgain)

    def score(group, first):
        for i in range(half):
            if i % chunk == 0:
                keys[(0 if first else KEY_CHUNKS // 2) + i // chunk].wait()
            s = group * half + i
            scores = lax.dot_general(
                qs[s].astype(BF16), ck[s], (((1,), (1,)), ((), ())), preferred_element_type=F32
            )
            exponent = jnp.where(position < lens[s], jnp.exp(scores), 0.0)
            den[s] = jnp.broadcast_to(
                jnp.sum(exponent, axis=-1, keepdims=True), den.shape[1:]
            )
            es[s] = exponent.astype(BF16)

    def attend(group, first):
        for i in range(half):
            if i % chunk == 0:
                vals[(0 if first else KEY_CHUNKS // 2) + i // chunk].wait()
            s = group * half + i
            att[s] = mm(es[s], cv[s])
        here = rows_of(group)
        kf = knew[here, :].reshape(half, 1, 2 * HEAD)
        vf = vnew[here, :].reshape(half, 1, vnew.shape[1])
        own_exp = jnp.exp(jnp.sum(qs[here] * kf, axis=-1, keepdims=True))
        att[here] = (att[here] + own_exp * vf) / (den[here] + own_exp)
        if first:
            proj[3].wait()
        heads = [
            (
                norm_scale(
                    att[here, 2 * h, :] - lam[h] * att[here, 2 * h + 1, :], head_gain
                )
                * HEAD_SCALE
            ).astype(BF16)
            for h in range(groups)
        ]
        return mm(jnp.concatenate(heads, axis=1), wo[...]).astype(BF16)

    score(other, True)
    for c in vals[2:]:
        c.start()
    part[...] = attend(other, True)
    for c in own:
        c.start()
    score(tp, False)
    pl.semaphore_wait(bar, n)
    swap = to_peer(part, part_in, 1, (me, other))
    swap.start()
    for h in range(PASSES):
        each_peer(lambda peer: to_peer(tabf.at[peer], tab.at[me], 0, (peer, tp)).start(), h)
    for i in (0, 1, 3, 4, 2, 5):
        swaps[i].start()
    partial = attend(tp, False)
    swap.wait()
    middle = resf[rows_of(tp), :] + (partial.astype(F32) + part_in[...].astype(F32))
    middle = middle.astype(BF16).astype(F32)
    mid[...] = middle
    xs[me] = norm_scale(middle, row_of(cgain)).astype(BF16)
    for k in range(PASSES):
        h = 2 * lax.rem(lax.div(my_part, 2) + k // 2, 2) + lax.rem(lax.rem(my_part, 2) + k % 2, 2)
        each_peer(
            lambda peer: to_peer(xs.at[me], xs.at[me], 2, (peer, tp), 4 + my_part).start(), h
        )
    for c in own:
        c.wait()
    for c in swaps:
        c.wait()
    blocks(tab, n - 1, 0).wait()

    count = reach * half

    def pass_over(h):
        for inside in (0, 1):

            @pl.when(my_part == h if inside else my_part != h)
            def _():
                blocks(xs, reach - inside, 2, 4 + h).wait_recv()

        here = slice(h * reach, (h + 1) * reach)
        xf = xs[here].astype(F32).reshape(count, width)
        x = xf.astype(BF16)
        switch = 1.0 / (
            1.0 + jnp.exp(-jnp.sum(xf * row_of(mixer), axis=-1, keepdims=True))
        )
        shape = (reach, half, tab.shape[2])
        token = lax.broadcasted_iota(jnp.int32, shape, 1) + tp * half
        spot = lax.broadcasted_iota(jnp.int32, shape, 2)
        weight = jnp.sum(
            jnp.where(spot == token, tab[here], 0.0), axis=-1, keepdims=True
        ).reshape(count, 1)
        total = None
        for gate, up, down, scale in ((eg, eu, ed, weight), (dg, du, dd, switch)):
            units = gate.shape[2]
            merge = units % 128 == 0
            for slots in ((0, 1),) if merge else ((0,), (1,)):
                gw = jnp.concatenate([gate[i] for i in slots], axis=1) if merge else gate[slots[0]]
                uw = jnp.concatenate([up[i] for i in slots], axis=1) if merge else up[slots[0]]
                dw = jnp.concatenate([down[i] for i in slots], axis=0) if merge else down[slots[0]]
                hidden = (silu(mm(x, gw)) * mm(x, uw) * scale).astype(BF16)
                term = mm(hidden, dw)
                total = term if total is None else total + term
        ys[here] = total.reshape(reach, half, width).astype(BF16)
        each_peer(lambda peer: to_peer(ys.at[peer], rs.at[me], 3, (peer, tp)).start(), h)

    for h in range(PASSES):
        pass_over(h)
    rs[me] = ys[me]
    blocks(xs, n - 1, 2).wait_send()
    blocks(ys, n - 1, 3).wait()
    ob[tp] = (mid[...] + jnp.sum(rs[...].astype(F32), axis=0)).astype(BF16)
    last = to_peer(ob.at[tp], ob.at[tp], 4, (me, other), 2)
    last.start()
    last.wait()
    out_ref[...] = ob[...].astype(F32).reshape(seqs, width).astype(BF16)


def hand_over(*refs):
    count = (len(refs) - 1) // 2
    sem = refs[-1]
    copies = [
        pltpu.make_async_copy(source, target, sem.at[i])
        for i, (source, target) in enumerate(zip(refs[:count], refs[count : 2 * count]))
    ]
    for c in copies:
        c.start()
    for c in copies:
        c.wait()


def per_device(
    n,
    residual_in,
    lengths,
    cache_keys,
    cache_values,
    attend_gain,
    query_proj,
    key_proj,
    value_proj,
    lambdas,
    head_gain,
    out_proj,
    channel_gain,
    routes,
    route_weight,
    expert_gate,
    expert_up,
    expert_down,
    dense_gate,
    dense_up,
    dense_down,
    dense_mixer,
):
    seqs, width = residual_in.shape
    _, kv_local, length, key_width = cache_keys.shape
    value_width = cache_values.shape[3]
    half = seqs // 2
    lanes = -(-seqs // 128) * 128
    rows = 8
    inverse = ROTARY_BASE ** (-np.arange(HEAD // 2, dtype=np.float32) / (HEAD // 2))
    inverse = jnp.asarray(np.tile(inverse.astype(np.float32), 4)[None, :])
    vmem = pl.BlockSpec(memory_space=pltpu.VMEM)
    hbm = pl.BlockSpec(memory_space=pltpu.HBM)

    def two(w):
        return pltpu.VMEM((2,) + w.shape, BF16)

    eg, eu, ed = expert_gate[0], expert_up[0], expert_down[0]
    small = (
        lengths,
        lambdas,
        inverse,
        residual_in,
        attend_gain,
        head_gain,
        channel_gain,
        dense_mixer,
        routes.T,
        route_weight.T,
    )
    big = (
        cache_keys.reshape(seqs, length, key_width),
        cache_values.reshape(seqs, length, value_width),
        query_proj,
        key_proj,
        value_proj,
        out_proj,
        eg,
        eu,
        ed,
        dense_gate,
        dense_up,
        dense_down,
    )
    dma = pltpu.SemaphoreType.DMA
    results = ((seqs, width), (seqs, key_width), (seqs, value_width))
    out, nk, nv = pl.pallas_call(
        functools.partial(kernel, n),
        out_shape=tuple(pltpu.VMEM(shape, BF16) for shape in results),
        in_specs=[hbm] * (len(small) + len(big)),
        out_specs=(vmem, vmem, vmem),
        scratch_shapes=[pltpu.SMEM(a.shape, a.dtype) for a in small[:2]]
        + [pltpu.VMEM(a.shape, a.dtype) for a in small[2:]]
        + [pltpu.VMEM(w.shape, BF16) for w in big[:6]]
        + [two(w) for w in big[6:]]
        + [
            pltpu.VMEM((seqs, 2 * HEAD), F32),
            pltpu.VMEM((seqs, width), F32),
            pltpu.VMEM((seqs, key_width), F32),
            pltpu.VMEM((seqs, value_width), F32),
            pltpu.VMEM((seqs, rows, key_width), F32),
            pltpu.VMEM((seqs, rows, length), BF16),
            pltpu.VMEM((seqs, rows, value_width), F32),
            pltpu.VMEM((seqs, rows, value_width), F32),
            pltpu.VMEM((half, width), BF16),
            pltpu.VMEM((half, width), BF16),
            pltpu.VMEM((half, width), F32),
            pltpu.VMEM((n, 1, lanes), F32),
            pltpu.VMEM((n, 1, lanes), F32),
            pltpu.VMEM((n, half, width), BF16),
            pltpu.VMEM((n, half, width), BF16),
            pltpu.VMEM((n, half, width), BF16),
            pltpu.VMEM((2, half, width), BF16),
            dma((len(small),)),
            dma((4,)),
            dma((KEY_CHUNKS,)),
            dma((KEY_CHUNKS,)),
            dma((6,)),
            dma((6,)),
            dma((6,)),
            dma((5,)),
            dma((4 + PASSES,)),
        ],
        compiler_params=pltpu.CompilerParams(
            collective_id=0, has_side_effects=True, vmem_limit_bytes=56 * 1024 * 1024
        ),
    )(*(pltpu.with_memory_space_constraint(a, pltpu.HBM) for a in small + big))
    out, nk, nv = pl.pallas_call(
        hand_over,
        out_shape=tuple(jax.ShapeDtypeStruct(shape, BF16) for shape in results),
        in_specs=[vmem] * 3,
        out_specs=(hbm, hbm, hbm),
        scratch_shapes=[dma((3,))],
        compiler_params=pltpu.CompilerParams(vmem_limit_bytes=1024 * 1024),
    )(out, nk, nv)
    return (
        out,
        nk.reshape(seqs, kv_local, key_width),
        nv.reshape(seqs, kv_local, value_width),
    )


def solution(mesh):
    return jax.shard_map(
        functools.partial(per_device, mesh.shape["ep"]),
        mesh=mesh,
        in_specs=(
            P("ep", None),
            P("ep"),
            P("ep", "tp", None, None),
            P("ep", "tp", None, None),
            P(),
            P(None, "tp"),
            P(None, "tp"),
            P(None, "tp"),
            P("tp"),
            P(),
            P("tp", None),
            P(),
            P("ep", None),
            P("ep", None),
            P("ep", None, "tp"),
            P("ep", None, "tp"),
            P("ep", "tp", None),
            P(None, ("ep", "tp")),
            P(None, ("ep", "tp")),
            P(("ep", "tp"), None),
            P(),
        ),
        out_specs=(P("ep", None), P("ep", "tp", None), P("ep", "tp", None)),
        check_vma=False,
    )
```

```python
import functools

import jax
import jax.numpy as jnp
import numpy as np
from jax import lax
from jax.experimental import pallas as pl
from jax.experimental.pallas import tpu as pltpu
from jax.sharding import PartitionSpec as P

HEAD = 64
NORM_EPSILON = 1e-06
ROTARY_BASE = 10000.0
HEAD_SCALE = 0.8
KEY_CHUNKS = 4
PASSES = 4
SEND_ORDER = ((0, 1, 2, 3), (1, 0, 3, 2), (2, 1, 0, 3), (3, 2, 1, 0))
GROUPS = ((0, 1), (1, 1), (2, 2))
MESH = pl.DeviceIdType.MESH
F32 = jnp.float32
BF16 = jnp.bfloat16


def norm_scale(vectors, gain_vector):
    mean_square = jnp.mean(vectors * vectors, axis=-1, keepdims=True)
    return vectors * lax.rsqrt(mean_square + NORM_EPSILON) * gain_vector


def mm(a, b):
    return jnp.dot(a, b, preferred_element_type=F32)


def row_of(ref):
    return ref[...].astype(F32).reshape(1, ref.shape[0])


def silu(v):
    return v / (1.0 + jnp.exp(-v))


def kernel(
    n,
    len_hbm,
    lam_hbm,
    inv_hbm,
    res_hbm,
    again_hbm,
    hgain_hbm,
    cgain_hbm,
    mixer_hbm,
    routes_hbm,
    rw_hbm,
    ck_hbm,
    cv_hbm,
    wq_hbm,
    wk_hbm,
    wv_hbm,
    wo_hbm,
    eg_hbm,
    eu_hbm,
    ed_hbm,
    dg_hbm,
    du_hbm,
    dd_hbm,
    out_ref,
    nk_ref,
    nv_ref,
    lens,
    lam,
    inv,
    res,
    again,
    hgain,
    cgain,
    mixer,
    routes_v,
    rw_v,
    ck,
    cv,
    wq,
    wk,
    wv,
    wo,
    eg,
    eu,
    ed,
    dg,
    du,
    dd,
    pos,
    resf,
    knew,
    vnew,
    qs,
    es,
    den,
    att,
    part,
    part_in,
    mid,
    tabf,
    tab,
    xs,
    ys,
    rs,
    ob,
    small_sem,
    proj_sem,
    key_sem,
    val_sem,
    own_sem,
    wsend,
    wrecv,
    sent,
    got,
):
    seqs, width = res.shape
    half = xs.shape[1]
    me = lax.axis_index("ep")
    tp = lax.axis_index("tp")
    other = 1 - tp
    chunk = seqs // KEY_CHUNKS
    reach = n // PASSES
    my_part = lax.div(me, reach)

    high, odd = lax.div(my_part, 2), lax.rem(my_part, 2)

    def in_order(table):
        near = [a + odd * (b - a) for a, b in zip(table[0], table[1])]
        far = [a + odd * (b - a) for a, b in zip(table[2], table[3])]
        return [a + high * (b - a) for a, b in zip(near, far)]

    def part_of(i):
        group = other if i < KEY_CHUNKS // 2 else tp
        return pl.ds(group * half + i % (KEY_CHUNKS // 2) * chunk, chunk)

    def rows_of(group):
        return pl.ds(pl.multiple_of(group * half, half), half)

    small = [
        pltpu.make_async_copy(a, b, small_sem.at[i])
        for i, (a, b) in enumerate(
            (
                (len_hbm, lens),
                (inv_hbm, inv),
                (res_hbm, res),
                (again_hbm, again),
                (routes_hbm, routes_v),
                (rw_hbm, rw_v),
                (lam_hbm, lam),
                (hgain_hbm, hgain),
                (cgain_hbm, cgain),
                (mixer_hbm, mixer),
            )
        )
    ]
    proj = [
        pltpu.make_async_copy(a, b, proj_sem.at[i])
        for i, (a, b) in enumerate(((wq_hbm, wq), (wk_hbm, wk), (wv_hbm, wv), (wo_hbm, wo)))
    ]
    keys = [
        pltpu.make_async_copy(ck_hbm.at[part_of(i)], ck.at[part_of(i)], key_sem.at[i])
        for i in range(KEY_CHUNKS)
    ]
    vals = [
        pltpu.make_async_copy(cv_hbm.at[part_of(i)], cv.at[part_of(i)], val_sem.at[i])
        for i in range(KEY_CHUNKS)
    ]
    weight_pairs = (
        (eg_hbm, eg),
        (eu_hbm, eu),
        (ed_hbm, ed),
        (dg_hbm, dg),
        (du_hbm, du),
        (dd_hbm, dd),
    )
    whole = own_sem.shape[0] == 1
    own = [
        pltpu.make_async_copy(a, b.at[0], own_sem.at[0 if whole else i])
        for i, (a, b) in enumerate(weight_pairs)
    ]
    for c in small[:4] + proj[:3] + small[4:]:
        c.start()

    keys[0].start()
    bar = pltpu.get_barrier_semaphore()
    pl.semaphore_signal(bar, inc=1, device_id=(me, other), device_id_type=MESH)

    def greet(k, c):
        pl.semaphore_signal(
            bar, inc=1, device_id=(lax.rem(me + k, n), tp), device_id_type=MESH
        )
        return c

    lax.fori_loop(1, n, greet, 0)

    keys[1].start()
    small[0].wait()
    for s in range(seqs):
        pos[s : s + 1, :] = jnp.full((1, 2 * HEAD), lens[s].astype(F32), F32)
    small[1].wait()
    angles = pos[...] * inv[...]
    cosine = jnp.cos(angles)
    lane = lax.broadcasted_iota(jnp.int32, (seqs, 2 * HEAD), 1)
    front = (lane % HEAD) < HEAD // 2
    sine = jnp.where(front, -1.0, 1.0) * jnp.sin(angles)

    def rotate(u):
        swapped = jnp.where(
            front,
            pltpu.roll(u, 2 * HEAD - HEAD // 2, 1),
            pltpu.roll(u, HEAD // 2, 1),
        )
        return (u * cosine + swapped * sine).astype(BF16)

    small[2].wait()
    small[3].wait()
    for c in vals[:2]:
        c.start()
    resf[...] = res[...].astype(F32)
    normed = norm_scale(resf[...], row_of(again)).astype(BF16)
    for c in small[4:]:
        c.wait()
    expert_row = lax.broadcasted_iota(jnp.int32, (n, 1, seqs), 0)
    routes = routes_v[...].reshape(-1, 1, 1, seqs)
    rweights = rw_v[...].reshape(-1, 1, 1, seqs)
    table = jnp.zeros((n, 1, seqs), F32)
    for k in range(routes.shape[0]):
        table = table + jnp.where(expert_row == routes[k], rweights[k], 0.0)
    tabf[...] = jnp.zeros_like(tabf)
    tabf[:, :, 0:seqs] = table
    tab[me] = tabf[me]
    for c in proj[:3]:
        c.wait()
    for c in keys[2:] + proj[3:]:
        c.start()
    queries = mm(normed, wq[...])
    new_keys = rotate(mm(normed, wk[...]))
    new_values = mm(normed, wv[...]).astype(BF16)
    nk_ref[...] = new_keys
    nv_ref[...] = new_values
    knew[...] = new_keys.astype(F32)
    vnew[...] = new_values.astype(F32)
    groups = queries.shape[1] // (2 * HEAD)
    rows = qs.shape[1]
    qs[...] = jnp.zeros_like(qs)
    for g in range(groups):
        turned = rotate(queries[:, g * 2 * HEAD : (g + 1) * 2 * HEAD]).astype(F32) * (
            HEAD**-0.5
        )
        for m in range(2):
            qs[:, 2 * g + m, :] = jnp.where(lane // HEAD == m, turned, 0.0)

    def to_peer(src, dst, k, peer, r=None):
        return pltpu.make_async_remote_copy(
            src_ref=src,
            dst_ref=dst,
            send_sem=sent.at[k],
            recv_sem=got.at[k if r is None else r],
            device_id=peer,
            device_id_type=MESH,
        )

    low = lax.rem(me, reach)

    def each_peer(send, h):
        if reach & (reach - 1) == 0 and reach <= 8:
            bits = [lax.rem(lax.div(low, 1 << b), 2) for b in range(reach.bit_length() - 1)]
            for k in range(reach - 1, 0, -1):
                send(
                    h * reach
                    + sum(
                        (1 << b) * (1 - bit if k >> b & 1 else bit)
                        for b, bit in enumerate(bits)
                    )
                )
        else:

            def step(k, c):
                send(h * reach + lax.rem(low + k, reach))
                return c

            lax.fori_loop(1, reach, step, 0)

        @pl.when(my_part != h)
        def _():
            send(h * reach + low)

    def blocks(buffer, count, k, r=None):
        block = buffer.at[pl.ds(0, count)]
        return to_peer(block, block, k, (me, other), r)

    swaps = [
        pltpu.make_async_remote_copy(
            src_ref=a,
            dst_ref=b.at[1],
            send_sem=wsend.at[0 if whole else i],
            recv_sem=wrecv.at[0 if whole else i],
            device_id=(me, other),
            device_id_type=MESH,
        )
        for i, (a, b) in enumerate(weight_pairs)
    ]
    position = lax.broadcasted_iota(jnp.int32, (rows, ck.shape[1]), 1)
    head_gain = row_of(hgain)

    def score(group, first):
        for i in range(half):
            if i % chunk == 0:
                keys[(0 if first else KEY_CHUNKS // 2) + i // chunk].wait()
            s = group * half + i
            scores = lax.dot_general(
                qs[s].astype(BF16), ck[s], (((1,), (1,)), ((), ())), preferred_element_type=F32
            )
            exponent = jnp.where(position < lens[s], jnp.exp(scores), 0.0)
            den[s] = jnp.broadcast_to(
                jnp.sum(exponent, axis=-1, keepdims=True), den.shape[1:]
            )
            es[s] = exponent.astype(BF16)

    def attend(group, first):
        for i in range(half):
            if i % chunk == 0:
                vals[(0 if first else KEY_CHUNKS // 2) + i // chunk].wait()
            s = group * half + i
            att[s] = mm(es[s], cv[s])
        here = rows_of(group)
        kf = knew[here, :].reshape(half, 1, 2 * HEAD)
        vf = vnew[here, :].reshape(half, 1, vnew.shape[1])
        own_exp = jnp.exp(jnp.sum(qs[here] * kf, axis=-1, keepdims=True))
        att[here] = (att[here] + own_exp * vf) / (den[here] + own_exp)
        if first:
            proj[3].wait()
        heads = [
            (
                norm_scale(
                    att[here, 2 * h, :] - lam[h] * att[here, 2 * h + 1, :], head_gain
                )
                * HEAD_SCALE
            ).astype(BF16)
            for h in range(groups)
        ]
        return mm(jnp.concatenate(heads, axis=1), wo[...]).astype(BF16)

    score(other, True)
    for c in vals[2:]:
        c.start()
    part[...] = attend(other, True)
    for c in own:
        c.start()
    swap = to_peer(part, part_in, 1, (me, other))

    def open_links():
        pl.semaphore_wait(bar, n)
        swap.start()
        for h in range(PASSES):
            each_peer(
                lambda peer: to_peer(
                    tabf.at[peer], tab.at[me], 0, (peer, tp), 4 + PASSES + my_part
                ).start(),
                h,
            )
        for i in (0, 1, 3, 4, 2, 5):
            swaps[i].start()

    pl.when(high == 1)(open_links)
    score(tp, False)
    pl.when(high == 0)(open_links)
    partial = attend(tp, False)
    swap.wait()
    middle = resf[rows_of(tp), :] + (partial.astype(F32) + part_in[...].astype(F32))
    middle = middle.astype(BF16).astype(F32)
    mid[...] = middle
    xs[me] = norm_scale(middle, row_of(cgain)).astype(BF16)
    for h in in_order(SEND_ORDER):
        each_peer(
            lambda peer: to_peer(xs.at[me], xs.at[me], 2, (peer, tp), 4 + my_part).start(), h
        )
    if whole:
        size = sum(a.shape[0] * a.shape[1] for a, _ in weight_pairs)
        like = ck.at[pl.ds(0, size // (ck.shape[1] * ck.shape[2]))]
        pltpu.make_async_copy(like, like, own_sem.at[0]).wait()
        pltpu.make_async_remote_copy(
            src_ref=like,
            dst_ref=like,
            send_sem=wsend.at[0],
            recv_sem=wrecv.at[0],
            device_id=(me, other),
            device_id_type=MESH,
        ).wait()
    else:
        for c in own + swaps:
            c.wait()
    blocks(tab, n - 1, 0).wait_send()

    def pass_over(first, parts):
        for h in range(first, first + parts):
            for inside in (0, 1):

                @pl.when(my_part == h if inside else my_part != h)
                def _():
                    blocks(tab, reach - inside, 0, 4 + PASSES + h).wait_recv()
                    blocks(xs, reach - inside, 2, 4 + h).wait_recv()

        here = slice(first * reach, (first + parts) * reach)
        count = parts * reach * half
        xf = xs[here].astype(F32).reshape(count, width)
        x = xf.astype(BF16)
        switch = 1.0 / (
            1.0 + jnp.exp(-jnp.sum(xf * row_of(mixer), axis=-1, keepdims=True))
        )
        shape = (parts * reach, half, tab.shape[2])
        token = lax.broadcasted_iota(jnp.int32, shape, 1) + tp * half
        spot = lax.broadcasted_iota(jnp.int32, shape, 2)
        weight = jnp.sum(
            jnp.where(spot == token, tab[here], 0.0), axis=-1, keepdims=True
        ).reshape(count, 1)
        total = None
        for gate, up, down, scale in ((eg, eu, ed, weight), (dg, du, dd, switch)):
            units = gate.shape[2]
            merge = units % 128 == 0
            for slots in ((0, 1),) if merge else ((0,), (1,)):
                gw = jnp.concatenate([gate[i] for i in slots], axis=1) if merge else gate[slots[0]]
                uw = jnp.concatenate([up[i] for i in slots], axis=1) if merge else up[slots[0]]
                dw = jnp.concatenate([down[i] for i in slots], axis=0) if merge else down[slots[0]]
                hidden = (silu(mm(x, gw)) * mm(x, uw) * scale).astype(BF16)
                term = mm(hidden, dw)
                total = term if total is None else total + term
        ys[here] = total.reshape(parts * reach, half, width).astype(BF16)
        for h in range(first, first + parts):
            each_peer(lambda peer: to_peer(ys.at[peer], rs.at[me], 3, (peer, tp)).start(), h)

    for first, parts in GROUPS:
        pass_over(first, parts)
    rs[me] = ys[me]
    blocks(xs, n - 1, 2).wait_send()
    blocks(ys, n - 1, 3).wait()
    ob[tp] = (mid[...] + jnp.sum(rs[...].astype(F32), axis=0)).astype(BF16)
    last = to_peer(ob.at[tp], ob.at[tp], 4, (me, other), 2)
    last.start()
    last.wait()
    out_ref[...] = ob[...].astype(F32).reshape(seqs, width).astype(BF16)


def hand_over(*refs):
    count = (len(refs) - 1) // 2
    sem = refs[-1]
    copies = [
        pltpu.make_async_copy(source, target, sem.at[i])
        for i, (source, target) in enumerate(zip(refs[:count], refs[count : 2 * count]))
    ]
    for c in copies:
        c.start()
    for c in copies:
        c.wait()


def per_device(
    n,
    residual_in,
    lengths,
    cache_keys,
    cache_values,
    attend_gain,
    query_proj,
    key_proj,
    value_proj,
    lambdas,
    head_gain,
    out_proj,
    channel_gain,
    routes,
    route_weight,
    expert_gate,
    expert_up,
    expert_down,
    dense_gate,
    dense_up,
    dense_down,
    dense_mixer,
):
    seqs, width = residual_in.shape
    _, kv_local, length, key_width = cache_keys.shape
    value_width = cache_values.shape[3]
    half = seqs // 2
    lanes = -(-seqs // 128) * 128
    rows = 8
    inverse = ROTARY_BASE ** (-np.arange(HEAD // 2, dtype=np.float32) / (HEAD // 2))
    inverse = jnp.asarray(np.tile(inverse.astype(np.float32), 4)[None, :])
    vmem = pl.BlockSpec(memory_space=pltpu.VMEM)
    hbm = pl.BlockSpec(memory_space=pltpu.HBM)

    def two(w):
        return pltpu.VMEM((2,) + w.shape, BF16)

    eg, eu, ed = expert_gate[0], expert_up[0], expert_down[0]
    small = (
        lengths,
        lambdas,
        inverse,
        residual_in,
        attend_gain,
        head_gain,
        channel_gain,
        dense_mixer,
        routes.T,
        route_weight.T,
    )
    big = (
        cache_keys.reshape(seqs, length, key_width),
        cache_values.reshape(seqs, length, value_width),
        query_proj,
        key_proj,
        value_proj,
        out_proj,
        eg,
        eu,
        ed,
        dense_gate,
        dense_up,
        dense_down,
    )
    dma = pltpu.SemaphoreType.DMA
    weights = big[6:]
    size = sum(w.size for w in weights)
    even = all(w.shape[1] % 128 == 0 for w in weights) and size % (length * key_width) == 0
    waits = 1 if even and size <= seqs * length * key_width else len(weights)
    results = ((seqs, width), (seqs, key_width), (seqs, value_width))
    out, nk, nv = pl.pallas_call(
        functools.partial(kernel, n),
        out_shape=tuple(pltpu.VMEM(shape, BF16) for shape in results),
        in_specs=[hbm] * (len(small) + len(big)),
        out_specs=(vmem, vmem, vmem),
        scratch_shapes=[pltpu.SMEM(a.shape, a.dtype) for a in small[:2]]
        + [pltpu.VMEM(a.shape, a.dtype) for a in small[2:]]
        + [pltpu.VMEM(w.shape, BF16) for w in big[:6]]
        + [two(w) for w in big[6:]]
        + [
            pltpu.VMEM((seqs, 2 * HEAD), F32),
            pltpu.VMEM((seqs, width), F32),
            pltpu.VMEM((seqs, key_width), F32),
            pltpu.VMEM((seqs, value_width), F32),
            pltpu.VMEM((seqs, rows, key_width), F32),
            pltpu.VMEM((seqs, rows, length), BF16),
            pltpu.VMEM((seqs, rows, value_width), F32),
            pltpu.VMEM((seqs, rows, value_width), F32),
            pltpu.VMEM((half, width), BF16),
            pltpu.VMEM((half, width), BF16),
            pltpu.VMEM((half, width), F32),
            pltpu.VMEM((n, 1, lanes), F32),
            pltpu.VMEM((n, 1, lanes), F32),
            pltpu.VMEM((n, half, width), BF16),
            pltpu.VMEM((n, half, width), BF16),
            pltpu.VMEM((n, half, width), BF16),
            pltpu.VMEM((2, half, width), BF16),
            dma((len(small),)),
            dma((4,)),
            dma((KEY_CHUNKS,)),
            dma((KEY_CHUNKS,)),
            dma((waits,)),
            dma((waits,)),
            dma((waits,)),
            dma((5,)),
            dma((4 + 2 * PASSES,)),
        ],
        compiler_params=pltpu.CompilerParams(
            collective_id=0, has_side_effects=True, vmem_limit_bytes=56 * 1024 * 1024
        ),
    )(*(pltpu.with_memory_space_constraint(a, pltpu.HBM) for a in small + big))
    out, nk, nv = pl.pallas_call(
        hand_over,
        out_shape=tuple(jax.ShapeDtypeStruct(shape, BF16) for shape in results),
        in_specs=[vmem] * 3,
        out_specs=(hbm, hbm, hbm),
        scratch_shapes=[dma((3,))],
        compiler_params=pltpu.CompilerParams(vmem_limit_bytes=1024 * 1024),
    )(out, nk, nv)
    return (
        out,
        nk.reshape(seqs, kv_local, key_width),
        nv.reshape(seqs, kv_local, value_width),
    )


def solution(mesh):
    return jax.shard_map(
        functools.partial(per_device, mesh.shape["ep"]),
        mesh=mesh,
        in_specs=(
            P("ep", None),
            P("ep"),
            P("ep", "tp", None, None),
            P("ep", "tp", None, None),
            P(),
            P(None, "tp"),
            P(None, "tp"),
            P(None, "tp"),
            P("tp"),
            P(),
            P("tp", None),
            P(),
            P("ep", None),
            P("ep", None),
            P("ep", None, "tp"),
            P("ep", None, "tp"),
            P("ep", "tp", None),
            P(None, ("ep", "tp")),
            P(None, ("ep", "tp")),
            P(("ep", "tp"), None),
            P(),
        ),
        out_specs=(P("ep", None), P("ep", "tp", None), P("ep", "tp", None)),
        check_vma=False,
    )
```

```python
import functools

import jax
import jax.numpy as jnp
import numpy as np
from jax import lax
from jax.experimental import pallas as pl
from jax.experimental.pallas import tpu as pltpu
from jax.sharding import PartitionSpec as P

HEAD = 64
NORM_EPSILON = 1e-06
ROTARY_BASE = 10000.0
HEAD_SCALE = 0.8
KEY_CHUNKS = 4
PASSES = 4
SEND_ORDER = ((0, 1, 2, 3), (1, 0, 3, 2), (2, 1, 0, 3), (3, 2, 1, 0))
GROUPS = ((0, 1), (1, 1), (2, 2))
MESH = pl.DeviceIdType.MESH
F32 = jnp.float32
BF16 = jnp.bfloat16


def norm_scale(vectors, gain_vector):
    mean_square = jnp.mean(vectors * vectors, axis=-1, keepdims=True)
    return vectors * lax.rsqrt(mean_square + NORM_EPSILON) * gain_vector


def mm(a, b):
    return jnp.dot(a, b, preferred_element_type=F32)


def row_of(ref):
    return ref[...].astype(F32).reshape(1, ref.shape[0])


def silu(v):
    return v / (1.0 + jnp.exp(-v))


def kernel(
    n,
    len_hbm,
    lam_hbm,
    inv_hbm,
    res_hbm,
    again_hbm,
    hgain_hbm,
    cgain_hbm,
    mixer_hbm,
    routes_hbm,
    rw_hbm,
    ck_hbm,
    cv_hbm,
    wq_hbm,
    wk_hbm,
    wv_hbm,
    wo_hbm,
    eg_hbm,
    eu_hbm,
    ed_hbm,
    dg_hbm,
    du_hbm,
    dd_hbm,
    out_ref,
    nk_ref,
    nv_ref,
    lens,
    lam,
    inv,
    res,
    again,
    hgain,
    cgain,
    mixer,
    routes_v,
    rw_v,
    ck,
    cv,
    wq,
    wk,
    wv,
    wo,
    eg,
    eu,
    ed,
    dg,
    du,
    dd,
    pos,
    resf,
    knew,
    vnew,
    qs,
    es,
    den,
    att,
    part,
    part_in,
    mid,
    tabf,
    tab,
    xs,
    ys,
    rs,
    ob,
    small_sem,
    proj_sem,
    key_sem,
    val_sem,
    own_sem,
    wsend,
    wrecv,
    sent,
    got,
):
    seqs, width = res.shape
    half = xs.shape[1]
    me = lax.axis_index("ep")
    tp = lax.axis_index("tp")
    other = 1 - tp
    chunk = seqs // KEY_CHUNKS
    reach = n // PASSES
    my_part = lax.div(me, reach)

    high, odd = lax.div(my_part, 2), lax.rem(my_part, 2)

    def in_order(table):
        near = [a + odd * (b - a) for a, b in zip(table[0], table[1])]
        far = [a + odd * (b - a) for a, b in zip(table[2], table[3])]
        return [a + high * (b - a) for a, b in zip(near, far)]

    def part_of(i):
        group = other if i < KEY_CHUNKS // 2 else tp
        return pl.ds(group * half + i % (KEY_CHUNKS // 2) * chunk, chunk)

    def rows_of(group):
        return pl.ds(pl.multiple_of(group * half, half), half)

    small = [
        pltpu.make_async_copy(a, b, small_sem.at[i])
        for i, (a, b) in enumerate(
            (
                (len_hbm, lens),
                (inv_hbm, inv),
                (res_hbm, res),
                (again_hbm, again),
                (routes_hbm, routes_v),
                (rw_hbm, rw_v),
                (lam_hbm, lam),
                (hgain_hbm, hgain),
                (cgain_hbm, cgain),
                (mixer_hbm, mixer),
            )
        )
    ]
    proj = [
        pltpu.make_async_copy(a, b, proj_sem.at[i])
        for i, (a, b) in enumerate(((wq_hbm, wq), (wk_hbm, wk), (wv_hbm, wv), (wo_hbm, wo)))
    ]
    keys = [
        pltpu.make_async_copy(ck_hbm.at[part_of(i)], ck.at[part_of(i)], key_sem.at[i])
        for i in range(KEY_CHUNKS)
    ]
    vals = [
        pltpu.make_async_copy(cv_hbm.at[part_of(i)], cv.at[part_of(i)], val_sem.at[i])
        for i in range(KEY_CHUNKS)
    ]
    weight_pairs = (
        (eg_hbm, eg),
        (eu_hbm, eu),
        (ed_hbm, ed),
        (dg_hbm, dg),
        (du_hbm, du),
        (dd_hbm, dd),
    )
    whole = own_sem.shape[0] == 1
    own = [
        pltpu.make_async_copy(a, b.at[0], own_sem.at[0 if whole else i])
        for i, (a, b) in enumerate(weight_pairs)
    ]
    for c in small[:4] + proj[:3] + small[4:]:
        c.start()

    keys[0].start()
    bar = pltpu.get_barrier_semaphore()
    pl.semaphore_signal(bar, inc=1, device_id=(me, other), device_id_type=MESH)

    def greet(k, c):
        pl.semaphore_signal(
            bar, inc=1, device_id=(lax.rem(me + k, n), tp), device_id_type=MESH
        )
        return c

    lax.fori_loop(1, n, greet, 0)

    keys[1].start()
    small[0].wait()
    for s in range(seqs):
        pos[s : s + 1, :] = jnp.full((1, 2 * HEAD), lens[s].astype(F32), F32)
    small[1].wait()
    angles = pos[...] * inv[...]
    cosine = jnp.cos(angles)
    lane = lax.broadcasted_iota(jnp.int32, (seqs, 2 * HEAD), 1)
    front = (lane % HEAD) < HEAD // 2
    sine = jnp.where(front, -1.0, 1.0) * jnp.sin(angles)

    def rotate(u):
        swapped = jnp.where(
            front,
            pltpu.roll(u, 2 * HEAD - HEAD // 2, 1),
            pltpu.roll(u, HEAD // 2, 1),
        )
        return (u * cosine + swapped * sine).astype(BF16)

    small[2].wait()
    small[3].wait()
    for c in vals[:2]:
        c.start()
    resf[...] = res[...].astype(F32)
    normed = norm_scale(resf[...], row_of(again)).astype(BF16)
    for c in small[4:]:
        c.wait()
    expert_row = lax.broadcasted_iota(jnp.int32, (n, 1, seqs), 0)
    routes = routes_v[...].reshape(-1, 1, 1, seqs)
    rweights = rw_v[...].reshape(-1, 1, 1, seqs)
    table = jnp.zeros((n, 1, seqs), F32)
    for k in range(routes.shape[0]):
        table = table + jnp.where(expert_row == routes[k], rweights[k], 0.0)
    tabf[...] = jnp.zeros_like(tabf)
    tabf[:, :, 0:seqs] = table
    tab[me] = tabf[me]
    for c in proj[:3]:
        c.wait()
    for c in keys[2:] + proj[3:]:
        c.start()
    queries = mm(normed, wq[...])
    new_keys = rotate(mm(normed, wk[...]))
    new_values = mm(normed, wv[...]).astype(BF16)
    nk_ref[...] = new_keys
    nv_ref[...] = new_values
    knew[...] = new_keys.astype(F32)
    vnew[...] = new_values.astype(F32)
    groups = queries.shape[1] // (2 * HEAD)
    rows = qs.shape[1]
    qs[...] = jnp.zeros_like(qs)
    for g in range(groups):
        turned = rotate(queries[:, g * 2 * HEAD : (g + 1) * 2 * HEAD]).astype(F32) * (
            HEAD**-0.5
        )
        for m in range(2):
            qs[:, 2 * g + m, :] = jnp.where(lane // HEAD == m, turned, 0.0)

    def to_peer(src, dst, k, peer, r=None):
        return pltpu.make_async_remote_copy(
            src_ref=src,
            dst_ref=dst,
            send_sem=sent.at[k],
            recv_sem=got.at[k if r is None else r],
            device_id=peer,
            device_id_type=MESH,
        )

    low = lax.rem(me, reach)

    def each_peer(send, h):
        if reach & (reach - 1) == 0 and reach <= 8:
            bits = [lax.rem(lax.div(low, 1 << b), 2) for b in range(reach.bit_length() - 1)]
            for k in range(reach - 1, 0, -1):
                send(
                    h * reach
                    + sum(
                        (1 << b) * (1 - bit if k >> b & 1 else bit)
                        for b, bit in enumerate(bits)
                    )
                )
        else:

            def step(k, c):
                send(h * reach + lax.rem(low + k, reach))
                return c

            lax.fori_loop(1, reach, step, 0)

        @pl.when(my_part != h)
        def _():
            send(h * reach + low)

    def blocks(buffer, count, k, r=None):
        block = buffer.at[pl.ds(0, count)]
        return to_peer(block, block, k, (me, other), r)

    swaps = [
        pltpu.make_async_remote_copy(
            src_ref=a,
            dst_ref=b.at[1],
            send_sem=wsend.at[0 if whole else i],
            recv_sem=wrecv.at[0 if whole else i],
            device_id=(me, other),
            device_id_type=MESH,
        )
        for i, (a, b) in enumerate(weight_pairs)
    ]
    position = lax.broadcasted_iota(jnp.int32, (rows, ck.shape[1]), 1)
    head_gain = row_of(hgain)

    def score(group, first):
        for i in range(half):
            if i % chunk == 0:
                keys[(0 if first else KEY_CHUNKS // 2) + i // chunk].wait()
            s = group * half + i
            scores = lax.dot_general(
                qs[s].astype(BF16), ck[s], (((1,), (1,)), ((), ())), preferred_element_type=F32
            )
            exponent = jnp.where(position < lens[s], jnp.exp(scores), 0.0)
            den[s] = jnp.broadcast_to(
                jnp.sum(exponent, axis=-1, keepdims=True), den.shape[1:]
            )
            es[s] = exponent.astype(BF16)

    def attend(group, first):
        for i in range(half):
            if i % chunk == 0:
                vals[(0 if first else KEY_CHUNKS // 2) + i // chunk].wait()
            s = group * half + i
            att[s] = mm(es[s], cv[s])
        here = rows_of(group)
        kf = knew[here, :].reshape(half, 1, 2 * HEAD)
        vf = vnew[here, :].reshape(half, 1, vnew.shape[1])
        own_exp = jnp.exp(jnp.sum(qs[here] * kf, axis=-1, keepdims=True))
        att[here] = (att[here] + own_exp * vf) / (den[here] + own_exp)
        if first:
            proj[3].wait()
        heads = [
            (
                norm_scale(
                    att[here, 2 * h, :] - lam[h] * att[here, 2 * h + 1, :], head_gain
                )
                * HEAD_SCALE
            ).astype(BF16)
            for h in range(groups)
        ]
        return mm(jnp.concatenate(heads, axis=1), wo[...]).astype(BF16)

    score(other, True)
    for c in vals[2:]:
        c.start()
    part[...] = attend(other, True)
    for c in own:
        c.start()
    swap = to_peer(part, part_in, 1, (me, other))

    def open_links():
        pl.semaphore_wait(bar, n)
        swap.start()
        for h in range(PASSES):
            each_peer(
                lambda peer: to_peer(
                    tabf.at[peer], tab.at[me], 0, (peer, tp), 4 + PASSES + my_part
                ).start(),
                h,
            )
        for i in (0, 1, 3, 4, 2, 5):
            swaps[i].start()

    pl.when(high == 1)(open_links)
    score(tp, False)
    pl.when(high == 0)(open_links)
    partial = attend(tp, False)
    swap.wait()
    middle = resf[rows_of(tp), :] + (partial.astype(F32) + part_in[...].astype(F32))
    middle = middle.astype(BF16).astype(F32)
    mid[...] = middle
    xs[me] = norm_scale(middle, row_of(cgain)).astype(BF16)
    def give_rows(h):
        each_peer(
            lambda peer: to_peer(xs.at[me], xs.at[me], 2, (peer, tp), 4 + my_part).start(), h
        )

    order = in_order(SEND_ORDER)
    for k, h in enumerate(order):
        if k < 2:
            give_rows(h)
        else:
            pl.when(tp == 0)(lambda: give_rows(h))
    if whole:
        size = sum(a.shape[0] * a.shape[1] for a, _ in weight_pairs)
        like = ck.at[pl.ds(0, size // (ck.shape[1] * ck.shape[2]))]
        pltpu.make_async_copy(like, like, own_sem.at[0]).wait()
        for h in order[2:]:
            pl.when(tp == 1)(lambda: give_rows(h))
        pltpu.make_async_remote_copy(
            src_ref=like,
            dst_ref=like,
            send_sem=wsend.at[0],
            recv_sem=wrecv.at[0],
            device_id=(me, other),
            device_id_type=MESH,
        ).wait()
    else:
        for h in order[2:]:
            pl.when(tp == 1)(lambda: give_rows(h))
        for c in own + swaps:
            c.wait()
    blocks(tab, n - 1, 0).wait_send()

    def pass_over(first, parts):
        for h in range(first, first + parts):
            for inside in (0, 1):

                @pl.when(my_part == h if inside else my_part != h)
                def _():
                    blocks(tab, reach - inside, 0, 4 + PASSES + h).wait_recv()
                    blocks(xs, reach - inside, 2, 4 + h).wait_recv()

        here = slice(first * reach, (first + parts) * reach)
        count = parts * reach * half
        xf = xs[here].astype(F32).reshape(count, width)
        x = xf.astype(BF16)
        switch = 1.0 / (
            1.0 + jnp.exp(-jnp.sum(xf * row_of(mixer), axis=-1, keepdims=True))
        )
        shape = (parts * reach, half, tab.shape[2])
        token = lax.broadcasted_iota(jnp.int32, shape, 1) + tp * half
        spot = lax.broadcasted_iota(jnp.int32, shape, 2)
        weight = jnp.sum(
            jnp.where(spot == token, tab[here], 0.0), axis=-1, keepdims=True
        ).reshape(count, 1)
        total = None
        for gate, up, down, scale in ((eg, eu, ed, weight), (dg, du, dd, switch)):
            units = gate.shape[2]
            merge = units % 128 == 0
            for slots in ((0, 1),) if merge else ((0,), (1,)):
                gw = jnp.concatenate([gate[i] for i in slots], axis=1) if merge else gate[slots[0]]
                uw = jnp.concatenate([up[i] for i in slots], axis=1) if merge else up[slots[0]]
                dw = jnp.concatenate([down[i] for i in slots], axis=0) if merge else down[slots[0]]
                hidden = (silu(mm(x, gw)) * mm(x, uw) * scale).astype(BF16)
                term = mm(hidden, dw)
                total = term if total is None else total + term
        ys[here] = total.reshape(parts * reach, half, width).astype(BF16)
        for h in range(first, first + parts):
            each_peer(lambda peer: to_peer(ys.at[peer], rs.at[me], 3, (peer, tp)).start(), h)

    for first, parts in GROUPS:
        pass_over(first, parts)
    rs[me] = ys[me]
    blocks(xs, n - 1, 2).wait_send()
    blocks(ys, n - 1, 3).wait()
    ob[tp] = (mid[...] + jnp.sum(rs[...].astype(F32), axis=0)).astype(BF16)
    last = to_peer(ob.at[tp], ob.at[tp], 4, (me, other), 2)
    last.start()
    last.wait()
    out_ref[...] = ob[...].astype(F32).reshape(seqs, width).astype(BF16)


def hand_over(*refs):
    count = (len(refs) - 1) // 2
    sem = refs[-1]
    copies = [
        pltpu.make_async_copy(source, target, sem.at[i])
        for i, (source, target) in enumerate(zip(refs[:count], refs[count : 2 * count]))
    ]
    for c in copies:
        c.start()
    for c in copies:
        c.wait()


def per_device(
    n,
    residual_in,
    lengths,
    cache_keys,
    cache_values,
    attend_gain,
    query_proj,
    key_proj,
    value_proj,
    lambdas,
    head_gain,
    out_proj,
    channel_gain,
    routes,
    route_weight,
    expert_gate,
    expert_up,
    expert_down,
    dense_gate,
    dense_up,
    dense_down,
    dense_mixer,
):
    seqs, width = residual_in.shape
    _, kv_local, length, key_width = cache_keys.shape
    value_width = cache_values.shape[3]
    half = seqs // 2
    lanes = -(-seqs // 128) * 128
    rows = 8
    inverse = ROTARY_BASE ** (-np.arange(HEAD // 2, dtype=np.float32) / (HEAD // 2))
    inverse = jnp.asarray(np.tile(inverse.astype(np.float32), 4)[None, :])
    vmem = pl.BlockSpec(memory_space=pltpu.VMEM)
    hbm = pl.BlockSpec(memory_space=pltpu.HBM)

    def two(w):
        return pltpu.VMEM((2,) + w.shape, BF16)

    eg, eu, ed = expert_gate[0], expert_up[0], expert_down[0]
    small = (
        lengths,
        lambdas,
        inverse,
        residual_in,
        attend_gain,
        head_gain,
        channel_gain,
        dense_mixer,
        routes.T,
        route_weight.T,
    )
    big = (
        cache_keys.reshape(seqs, length, key_width),
        cache_values.reshape(seqs, length, value_width),
        query_proj,
        key_proj,
        value_proj,
        out_proj,
        eg,
        eu,
        ed,
        dense_gate,
        dense_up,
        dense_down,
    )
    dma = pltpu.SemaphoreType.DMA
    weights = big[6:]
    size = sum(w.size for w in weights)
    even = all(w.shape[1] % 128 == 0 for w in weights) and size % (length * key_width) == 0
    waits = 1 if even and size <= seqs * length * key_width else len(weights)
    results = ((seqs, width), (seqs, key_width), (seqs, value_width))
    out, nk, nv = pl.pallas_call(
        functools.partial(kernel, n),
        out_shape=tuple(pltpu.VMEM(shape, BF16) for shape in results),
        in_specs=[hbm] * (len(small) + len(big)),
        out_specs=(vmem, vmem, vmem),
        scratch_shapes=[pltpu.SMEM(a.shape, a.dtype) for a in small[:2]]
        + [pltpu.VMEM(a.shape, a.dtype) for a in small[2:]]
        + [pltpu.VMEM(w.shape, BF16) for w in big[:6]]
        + [two(w) for w in big[6:]]
        + [
            pltpu.VMEM((seqs, 2 * HEAD), F32),
            pltpu.VMEM((seqs, width), F32),
            pltpu.VMEM((seqs, key_width), F32),
            pltpu.VMEM((seqs, value_width), F32),
            pltpu.VMEM((seqs, rows, key_width), F32),
            pltpu.VMEM((seqs, rows, length), BF16),
            pltpu.VMEM((seqs, rows, value_width), F32),
            pltpu.VMEM((seqs, rows, value_width), F32),
            pltpu.VMEM((half, width), BF16),
            pltpu.VMEM((half, width), BF16),
            pltpu.VMEM((half, width), F32),
            pltpu.VMEM((n, 1, lanes), F32),
            pltpu.VMEM((n, 1, lanes), F32),
            pltpu.VMEM((n, half, width), BF16),
            pltpu.VMEM((n, half, width), BF16),
            pltpu.VMEM((n, half, width), BF16),
            pltpu.VMEM((2, half, width), BF16),
            dma((len(small),)),
            dma((4,)),
            dma((KEY_CHUNKS,)),
            dma((KEY_CHUNKS,)),
            dma((waits,)),
            dma((waits,)),
            dma((waits,)),
            dma((5,)),
            dma((4 + 2 * PASSES,)),
        ],
        compiler_params=pltpu.CompilerParams(
            collective_id=0, has_side_effects=True, vmem_limit_bytes=56 * 1024 * 1024
        ),
    )(*(pltpu.with_memory_space_constraint(a, pltpu.HBM) for a in small + big))
    out, nk, nv = pl.pallas_call(
        hand_over,
        out_shape=tuple(jax.ShapeDtypeStruct(shape, BF16) for shape in results),
        in_specs=[vmem] * 3,
        out_specs=(hbm, hbm, hbm),
        scratch_shapes=[dma((3,))],
        compiler_params=pltpu.CompilerParams(vmem_limit_bytes=1024 * 1024),
    )(out, nk, nv)
    return (
        out,
        nk.reshape(seqs, kv_local, key_width),
        nv.reshape(seqs, kv_local, value_width),
    )


def solution(mesh):
    return jax.shard_map(
        functools.partial(per_device, mesh.shape["ep"]),
        mesh=mesh,
        in_specs=(
            P("ep", None),
            P("ep"),
            P("ep", "tp", None, None),
            P("ep", "tp", None, None),
            P(),
            P(None, "tp"),
            P(None, "tp"),
            P(None, "tp"),
            P("tp"),
            P(),
            P("tp", None),
            P(),
            P("ep", None),
            P("ep", None),
            P("ep", None, "tp"),
            P("ep", None, "tp"),
            P("ep", "tp", None),
            P(None, ("ep", "tp")),
            P(None, ("ep", "tp")),
            P(("ep", "tp"), None),
            P(),
        ),
        out_specs=(P("ep", None), P("ep", "tp", None), P("ep", "tp", None)),
        check_vma=False,
    )
```
